128 devices in a mesh: ra: 16 (over z, y), cb: 8 (over x, core).
Axes of the slice: x: 4, y: 4, z: 4, core: 2. Of those that a mesh axis runs over, the one named last changes fastest.
Arguments:
- tokens: bfloat16 [4, 128, 4096], P(None, None, 'ra'), may hold values from -64 to 64
- norm_gain: float32 [2, 4096], P(None, 'ra'), may hold values from 0.1 to 1.9
- gate_weight: bfloat16 [2, 4096, 11264], P(None, 'ra', 'cb'), may hold values from -0.09375 to 0.09375
- up_weight: bfloat16 [2, 4096, 11264], P(None, 'ra', 'cb'), may hold values from -0.09375 to 0.09375
- gate_taps: float32 [2, 3, 11264], P(None, None, 'cb'), may hold values from -3 to 3
- up_taps: float32 [2, 3, 11264], P(None, None, 'cb'), may hold values from -3 to 3
- gate_bias: float32 [2, 11264], P(None, 'cb'), may hold values from -3 to 3
- up_bias: float32 [2, 11264], P(None, 'cb'), may hold values from -3 to 3
- down_weight: bfloat16 [2, 11264, 4096], P(None, 'cb', 'ra'), may hold values from -0.0546875 to 0.0546875
Outputs:
- mixed: bfloat16 [4, 128, 4096], P(None, None, 'ra')
The draws below stay inside these ranges and needn't reach their ends.
All inputs are finite; a program needn't handle non-finite values.
Results may differ from the reference program's by a relative error of at most 0.03.
Values may be sent and summed in bfloat16 or wider, within the bound.
No kernel may reach another device: no remote copies, remote signals or barrier semaphores. Data moves between devices by JAX's collectives and lax.ppermute only.
A program may use at most 64 MiB of HBM per device.

```python
import jax
import jax.numpy as jnp
from jax import lax

D = 4096
FF = 11264
KERNEL = 3
LAYERS = 2
SEQS = 4
LEN = 128


def draw_tokens(key, part):
    key_base, key_scale, key_rows, key_common = jax.random.split(key, 4)
    width = D // 32
    noise = jnp.clip(jax.random.normal(key_base, (SEQS, LEN, D), jnp.float32), -6.0, 6.0)
    row_scale = jnp.exp(jax.random.uniform(key_rows, (SEQS, LEN, 1), jnp.float32, -0.5, 0.5))
    scales = jnp.exp(jax.random.uniform(key_scale, (32,), jnp.float32, -1.4, 1.4))
    columns = jnp.repeat(scales, width)
    return jnp.clip(noise * columns * row_scale, -64.0, 64.0).astype(jnp.bfloat16)


def block_scale(rng, shape, cuts, least, largest):
    loudness = 1.0
    for position, parts in cuts:
        heights = jax.random.uniform(jax.random.fold_in(jax.random.fold_in(rng, 6), position), (parts,), jnp.float32, least / len(cuts), largest / len(cuts))
        loudness = loudness * jnp.repeat(jnp.exp(heights), shape[position] // parts).reshape((-1,) + (1,) * (len(shape) - 1 - position))
    return loudness


def centred(stream_key, shape, deviation, most, shards=(), dtype=jnp.bfloat16):
    gain = block_scale(stream_key, shape, shards, -0.22, 0.18) if shards else 1.0
    values = jax.random.normal(stream_key, shape, jnp.float32) * deviation * gain
    return jnp.minimum(jnp.maximum(values, -most), most).astype(dtype)


def setup_inputs(seed: int = 0) -> dict:
    arg_keys = jax.random.split(jax.random.key(seed), 10)
    tokens = draw_tokens(jax.random.fold_in(arg_keys[9], 71), 0)
    norm_gain = jnp.clip(1.0 + 0.18 * jax.random.normal(arg_keys[1], (LAYERS, D), jnp.float32), 0.1, 1.9)
    gate_weight = centred(arg_keys[2], (LAYERS, D, FF), D ** -0.5, 0.09375, ((1, 16), (2, 8)))
    up_weight = centred(arg_keys[3], (LAYERS, D, FF), D ** -0.5, 0.09375, ((1, 16), (2, 8)))
    gate_taps = centred(arg_keys[4], (LAYERS, KERNEL, FF), 0.6, 3.0, ((2, 8),), jnp.float32)
    up_taps = centred(arg_keys[5], (LAYERS, KERNEL, FF), 0.6, 3.0, ((2, 8),), jnp.float32)
    gate_bias = centred(arg_keys[6], (LAYERS, FF), 0.5, 3.0, ((1, 8),), jnp.float32)
    up_bias = centred(arg_keys[7], (LAYERS, FF), 0.5, 3.0, ((1, 8),), jnp.float32)
    down_weight = centred(arg_keys[8], (LAYERS, FF, D), FF ** -0.5, 0.0546875, ((1, 8), (2, 16)))
    return {"tokens": tokens, "norm_gain": norm_gain, "gate_weight": gate_weight, "up_weight": up_weight, "gate_taps": gate_taps, "up_taps": up_taps, "gate_bias": gate_bias, "up_bias": up_bias, "down_weight": down_weight}


eps = 1e-06
resid_scale = 0.5

def causal_conv(projected, kernel, offsets):
    values = projected.astype(jnp.float32).reshape(SEQS, LEN, FF)
    padded = jnp.pad(values, ((0, 0), (KERNEL - 1, 0), (0, 0)))
    result = offsets
    for tap_idx in range(KERNEL):
        result = result + kernel[tap_idx] * padded[:, tap_idx:tap_idx + LEN]
    return result.reshape(SEQS * LEN, FF)

def reference(tokens, norm_gain, gate_weight, up_weight, gate_taps, up_taps, gate_bias, up_bias, down_weight):
    carried = tokens.reshape(SEQS * LEN, D).astype(jnp.float32)
    for layer_idx in range(LAYERS):
        row_squares = lax.optimization_barrier(jnp.sum(carried * carried, axis=1))
        scaled = (carried * norm_gain[layer_idx]).astype(jnp.bfloat16)
        inverse = lax.rsqrt(row_squares / D + eps)
        gate_pre = (jnp.dot(scaled, gate_weight[layer_idx], preferred_element_type=jnp.float32) * inverse[:, None]).astype(jnp.bfloat16)
        up_pre = (jnp.dot(scaled, up_weight[layer_idx], preferred_element_type=jnp.float32) * inverse[:, None]).astype(jnp.bfloat16)
        gate_conv = causal_conv(gate_pre, gate_taps[layer_idx], gate_bias[layer_idx])
        up_conv = causal_conv(up_pre, up_taps[layer_idx], up_bias[layer_idx])
        hidden = (jax.nn.silu(gate_conv) * up_conv).astype(jnp.bfloat16)
        branch = jnp.dot(hidden, down_weight[layer_idx], preferred_element_type=jnp.float32)
        carried = resid_scale * carried + branch
    return carried.astype(jnp.bfloat16).reshape(SEQS, LEN, D)
```

```python
import jax
import jax.numpy as jnp
from jax import lax
from jax.sharding import PartitionSpec as P

D = 4096
KERNEL = 3
LAYERS = 2
SIDE = 4
AXES = ("ra", "cb")

eps = 1e-06
resid_scale = 0.5


def pairs(move):
    out = []
    for z in range(SIDE):
        for y in range(SIDE):
            for x in range(SIDE):
                for core in range(2):
                    to_z, to_y, to_x, to_core = move(z, y, x, core)
                    here = ((z * SIDE + y) * SIDE + x) * 2 + core
                    there = ((to_z * SIDE + to_y) * SIDE + to_x) * 2 + to_core
                    out.append((here, there))
    return out


def to_twin(value):
    return lax.ppermute(value, AXES, pairs(lambda z, y, x, c: (z, y, x, 1 - c)))


def along_first(value, d):
    move = lambda z, y, x, c: (z, y ^ d, x, c) if c == 0 else (z ^ d, y, x, c)
    return lax.ppermute(value, AXES, pairs(move))


def along_second(value, d):
    move = lambda z, y, x, c: (z ^ d, y, x, c) if c == 0 else (z, y ^ d, x, c)
    return lax.ppermute(value, AXES, pairs(move))


def along_x(value, d):
    return lax.ppermute(value, AXES, pairs(lambda z, y, x, c: (z, y, x ^ d, c)))


def halves(value):
    high = value.astype(jnp.bfloat16)
    low = (value - high.astype(jnp.float32)).astype(jnp.bfloat16)
    return jnp.stack([high, low])


def causal_conv(values, taps, bias):
    length = values.shape[2]
    padded = jnp.pad(values, ((0, 0), (0, 0), (KERNEL - 1, 0)))
    result = bias[:, None, None]
    for tap in range(KERNEL):
        result = result + taps[tap][:, None, None] * padded[:, :, tap : tap + length]
    return result


def per_device(
    tokens, norm_gain, gate_weight, up_weight, gate_taps, up_taps, gate_bias, up_bias, down_weight
):
    seqs, length, width = tokens.shape
    core = lax.axis_index("cb") % 2
    row, col = lax.axis_index("ra") // SIDE, lax.axis_index("ra") % SIDE
    first = jnp.where(core == 0, col, row)
    second = jnp.where(core == 0, row, col)
    own_seqs = seqs // 2
    rows = own_seqs * length
    cols = gate_weight.shape[2]
    quarter = cols // 2
    share = quarter // SIDE

    mine = lax.dynamic_slice_in_dim(tokens, core * own_seqs, own_seqs, 0)
    carried = mine.reshape(rows, width).T.astype(jnp.float32)

    both = []
    small = []
    for l in range(LAYERS):
        own = jnp.stack([gate_weight[l], up_weight[l]])
        both.append(jnp.stack([own, to_twin(own)]))
        own = jnp.stack(
            [
                jnp.concatenate([gate_taps[l], gate_bias[l][None]]),
                jnp.concatenate([up_taps[l], up_bias[l][None]]),
            ]
        )
        small.append(jnp.stack([own, to_twin(own)]))
    downs = []
    for l in range(LAYERS):
        downs.append(jnp.concatenate([down_weight[l], to_twin(down_weight[l])]))

    for l in range(LAYERS):
        squares = halves(jnp.sum(carried * carried, axis=0))
        scaled = (carried * norm_gain[l][:, None]).astype(jnp.bfloat16)

        def piece(d):
            target = first ^ d
            weights = lax.dynamic_slice(
                both[l], (target // 2, 0, 0, (target % 2) * quarter), (1, 2, width, quarter)
            )[0]
            part = lax.dot_general(
                weights, scaled, (((1,), (0,)), ((), ())), preferred_element_type=jnp.float32
            )
            part = part.astype(jnp.bfloat16).reshape(2 * quarter, rows)
            return jnp.concatenate([part, squares])

        parts = [along_first(piece(d), d) for d in (1, 3, 2)] + [piece(0)]
        total = sum(p.astype(jnp.float32) for p in parts)
        sums = total[: 2 * quarter].reshape(2, SIDE, share, rows)
        squares = halves(total[2 * quarter] + total[2 * quarter + 1])

        def piece2(d):
            part = lax.dynamic_index_in_dim(sums, second ^ d, 1, keepdims=False)
            return jnp.concatenate([part.reshape(2 * share, rows).astype(jnp.bfloat16), squares])

        parts = [along_second(piece2(d), d) for d in (1, 3, 2)] + [piece2(0)]
        total = sum(p.astype(jnp.float32) for p in parts)
        row_squares = total[2 * share] + total[2 * share + 1]
        inverse = lax.rsqrt(row_squares / D + eps)
        pre = (total[: 2 * share] * inverse[None]).astype(jnp.bfloat16).astype(jnp.float32)
        pre = pre.reshape(2, share, own_seqs, length)
        start = (first % 2) * quarter + second * share
        tb = lax.dynamic_slice(
            small[l], (first // 2, 0, 0, start), (1, 2, KERNEL + 1, share)
        )[0]
        gate = causal_conv(pre[0], tb[0, :KERNEL], tb[0, KERNEL])
        up = causal_conv(pre[1], tb[1, :KERNEL], tb[1, KERNEL])
        hidden = (jax.nn.silu(gate) * up).astype(jnp.bfloat16).reshape(share, rows)

        got = [hidden] + [along_second(hidden, d) for d in (1, 2, 3)]
        block = jnp.zeros((SIDE, share, rows), jnp.bfloat16)
        for d in range(SIDE):
            block = lax.dynamic_update_index_in_dim(block, got[d], second ^ d, 0)
        block = block.reshape(quarter, rows)
        got = [along_first(block, d) for d in (1, 3, 2)] + [block]
        branch = 0
        for d, part in zip((1, 3, 2, 0), got):
            rows_of = lax.dynamic_slice_in_dim(downs[l], (first ^ d) * quarter, quarter, 0)
            branch = branch + lax.dot_general(
                rows_of, part, (((0,), (0,)), ((), ())), preferred_element_type=jnp.float32
            )
        branch = branch.astype(jnp.bfloat16)
        got = [branch] + [along_x(branch, d) for d in (1, 2, 3)]
        got = [g.astype(jnp.float32) for g in got]
        branch = (got[0] + got[1]) + (got[2] + got[3])
        carried = resid_scale * carried + branch
    mine = carried.astype(jnp.bfloat16).T.reshape(own_seqs, length, width)
    other = to_twin(mine)
    low = jnp.where(core == 0, mine, other)
    high = jnp.where(core == 0, other, mine)
    return jnp.concatenate([low, high])


def solution(mesh):
    in_specs = (
        P(None, None, "ra"),
        P(None, "ra"),
        P(None, "ra", "cb"),
        P(None, "ra", "cb"),
        P(None, None, "cb"),
        P(None, None, "cb"),
        P(None, "cb"),
        P(None, "cb"),
        P(None, "cb", "ra"),
    )
    out_specs = P(None, None, "ra")
    return jax.shard_map(
        per_device, mesh=mesh, in_specs=in_specs, out_specs=out_specs, check_vma=False
    )
```

```python
import jax
import jax.numpy as jnp
from jax import lax
from jax.experimental import pallas as pl
from jax.experimental.pallas import tpu as pltpu
from jax.sharding import PartitionSpec as P

D = 4096
KERNEL = 3
LAYERS = 2
SIDE = 4
EXTRA = 16
AXES = ("ra", "cb")
BF16 = jnp.bfloat16
F32 = jnp.float32

eps = 1e-06
resid_scale = 0.5


def pairs(move):
    out = []
    for z in range(SIDE):
        for y in range(SIDE):
            for x in range(SIDE):
                for core in range(2):
                    to_z, to_y, to_x, to_core = move(z, y, x, core)
                    here = ((z * SIDE + y) * SIDE + x) * 2 + core
                    there = ((to_z * SIDE + to_y) * SIDE + to_x) * 2 + to_core
                    out.append((here, there))
    return out


def to_twin(value):
    return lax.ppermute(value, AXES, pairs(lambda z, y, x, c: (z, y, x, 1 - c)))


def along_first(value, d):
    move = lambda z, y, x, c: (z, y ^ d, x, c) if c == 0 else (z ^ d, y, x, c)
    return lax.ppermute(value, AXES, pairs(move))


def along_second(value, d):
    move = lambda z, y, x, c: (z ^ d, y, x, c) if c == 0 else (z, y ^ d, x, c)
    return lax.ppermute(value, AXES, pairs(move))


def along_x(value, d):
    return lax.ppermute(value, AXES, pairs(lambda z, y, x, c: (z, y, x ^ d, c)))


SMEM = pl.BlockSpec(memory_space=pltpu.SMEM)
VMEM = pl.BlockSpec(memory_space=pltpu.VMEM)


def local(kernel, name, outs, at, *args, flops=10**9):
    many = isinstance(outs, list)
    moved = sum(a.size * a.dtype.itemsize for a in args)
    return pl.pallas_call(
        kernel,
        in_specs=[SMEM] + [VMEM] * len(args),
        out_specs=[VMEM] * len(outs) if many else VMEM,
        out_shape=outs,
        compiler_params=pltpu.CompilerParams(vmem_limit_bytes=16 * 2**20),
        cost_estimate=pl.CostEstimate(flops=flops, bytes_accessed=moved, transcendentals=0),
        name=name,
    )(at, *args)


def array(shape, dtype):
    return jax.ShapeDtypeStruct(shape, dtype)


def turn_in(at, gate_weight, up_weight, l):
    _, width, cols = gate_weight.shape
    share = cols // (2 * SIDE)

    def kernel(at, gate, up, out):
        gate_t, up_t = gate[l].T, up[l].T
        for block in range(2 * SIDE):
            rows = slice(block * share, (block + 1) * share)
            out[2 * block * share : (2 * block + 1) * share] = gate_t[rows]
            out[(2 * block + 1) * share : (2 * block + 2) * share] = up_t[rows]

    return local(kernel, "turn_in", array((2 * cols, width), BF16), at, gate_weight, up_weight)


def turn_down(at, down_weight, l):
    _, cols, width = down_weight.shape
    quarter = cols // 2

    def kernel(at, weights, out):
        for h in range(2):
            out[h] = weights[l, h * quarter : (h + 1) * quarter].T

    return local(kernel, "turn_down", array((2, width, quarter), BF16), at, down_weight)


def split_rows(row_sum):
    high = row_sum.astype(BF16).astype(F32)
    low = row_sum - high
    shape = (EXTRA, row_sum.shape[1])
    row = lax.broadcasted_iota(jnp.int32, shape, 0)
    high = jnp.broadcast_to(high, shape)
    low = jnp.broadcast_to(low, shape)
    return jnp.where(row == 0, high, jnp.where(row == 1, low, 0.0)).astype(BF16)


def begin(value, gain, l, carried, scaled, squares):
    column = jnp.broadcast_to(gain[l : l + 1], (8, gain.shape[1])).T[:, :1]
    carried[...] = value
    scaled[...] = (value * column).astype(BF16)
    squares[...] = split_rows(jnp.sum(value * value, axis=0, keepdims=True))


def block_arrays(width, rows):
    return [array((width, rows), F32), array((width, rows), BF16), array((EXTRA, rows), BF16)]


def first_block(at, tokens, gain):
    seqs, length, width = tokens.shape
    own = seqs // 2

    def kernel(at, tokens, gain, *outs):
        mine = tokens[pl.ds(at[0] * own, own)].reshape(own * length, width)
        begin(mine.astype(F32).T, gain, 0, *outs)

    return local(kernel, "first_block", block_arrays(width, own * length), at, tokens, gain)


def added(carried, parts):
    a, b, c, d = (p[...].astype(F32) for p in parts)
    return resid_scale * carried[...] + ((a + b) + (c + d))


def next_block(at, carried, parts, gain, l):
    def kernel(at, carried, a, b, c, d, gain, *outs):
        begin(added(carried, (a, b, c, d)), gain, l, *outs)

    return local(kernel, "next_block", block_arrays(*carried.shape), at, carried, *parts, gain)


def last_block(at, carried, parts, seqs, length):
    def kernel(at, carried, a, b, c, d, out):
        out[...] = added(carried, (a, b, c, d)).T.astype(BF16).reshape(out.shape)

    out = array((seqs, length, carried.shape[0]), BF16)
    return local(kernel, "last_block", out, at, carried, *parts)


def joined(at, mine, other):
    seqs, length, width = mine.shape

    def kernel(at, mine, other, out):
        out[pl.ds(at[0] * seqs, seqs)] = mine[...]
        out[pl.ds((1 - at[0]) * seqs, seqs)] = other[...]

    return local(kernel, "joined", array((2 * seqs, length, width), BF16), at, mine, other)


def piece(at, d, own, other, scaled, squares):
    cols, width = own.shape
    rows = scaled.shape[1]
    block = cols // (2 * SIDE)

    def kernel(at, own, other, scaled, squares, out):
        target = at[1] ^ d
        acts = scaled[...]
        out[SIDE * block :] = squares[...]

        def store(weights):
            for j in range(SIDE):
                start = pl.multiple_of((target % 2) * (SIDE * block) + j * block, 16)
                part = jnp.dot(weights[pl.ds(start, block)], acts, preferred_element_type=F32)
                out[j * block : (j + 1) * block] = part.astype(BF16)

        @pl.when(target < 2)
        def _():
            store(own)

        @pl.when(target >= 2)
        def _():
            store(other)

    out = array((cols // 2 + EXTRA, rows), BF16)
    flops = cols * width * rows
    return local(kernel, "piece", out, at, own, other, scaled, squares, flops=flops)


def fold(at, parts, order):
    total, rows = parts[0].shape
    block = (total - EXTRA) // SIDE

    def kernel(at, *refs):
        parts, outs = refs[:SIDE], refs[SIDE:]

        def total_of(rows):
            a, b, c, d = (r[rows].astype(F32) for r in parts)
            return (a + b) + (c + d)

        extra = total_of(pl.ds(SIDE * block, EXTRA))
        extra = split_rows(extra[0:1] + extra[1:2])
        for d, out in zip(order, outs):
            start = pl.multiple_of((at[2] ^ d) * block, 16)
            out[:block] = total_of(pl.ds(start, block)).astype(BF16)
            out[block:] = extra

    outs = [array((block + EXTRA, rows), BF16)] * SIDE
    return local(kernel, "fold", outs, at, *parts)


def gated(at, parts, small, length):
    total, rows = parts[0].shape
    share = (total - EXTRA) // 2

    def kernel(at, a, b, c, d, small, out):
        value = (a[...].astype(F32) + b[...].astype(F32)) + (c[...].astype(F32) + d[...].astype(F32))
        row_squares = value[2 * share : 2 * share + 1] + value[2 * share + 1 : 2 * share + 2]
        inverse = lax.rsqrt(row_squares / D + eps)
        pre = (value[: 2 * share] * inverse).astype(BF16).astype(F32)
        lane = lax.broadcasted_iota(jnp.int32, (2 * share, length), 1)
        coef = small[...]
        for s in range(rows // length):
            now = pre[:, s * length : (s + 1) * length]
            one = jnp.where(lane >= 1, pltpu.roll(now, 1, 1), 0.0)
            two = jnp.where(lane >= 2, pltpu.roll(now, 2, 1), 0.0)
            conv = coef[:, 3:4] + coef[:, 0:1] * two + coef[:, 1:2] * one + coef[:, 2:3] * now
            gate, up = conv[:share], conv[share:]
            result = gate / (1.0 + jnp.exp(-gate)) * up
            out[:, s * length : (s + 1) * length] = result.astype(BF16)

    return local(kernel, "gated", array((share, rows), BF16), at, *parts, small)


def collected(at, parts):
    share, rows = parts[0].shape

    def kernel(at, *refs):
        for d in range(SIDE):
            start = pl.multiple_of((at[2] ^ d) * share, 16)
            refs[SIDE][pl.ds(start, share)] = refs[d][...]

    return local(kernel, "collected", array((SIDE * share, rows), BF16), at, *parts)


def down(at, ds, own, other, blocks, carry, dtype):
    _, width, quarter = own.shape
    n, rows = len(blocks), blocks[0].shape[1]
    carries = [] if carry is None else [carry]

    def kernel(at, own, other, *refs):
        blocks, rest = refs[:n], refs[n:]
        total = rest[0][...] if len(rest) == 2 else 0.0
        for d, block in zip(ds, blocks):
            target = at[1] ^ d
            half = target % 2
            chosen = jnp.where(target < 2, own[half], other[half])
            total = total + jnp.dot(chosen, block[...], preferred_element_type=F32)
        rest[-1][...] = total.astype(dtype)

    flops = 2 * n * width * quarter * rows
    out = array((width, rows), dtype)
    return local(kernel, "down", out, at, own, other, *blocks, *carries, flops=flops)


def per_device(
    tokens, norm_gain, gate_weight, up_weight, gate_taps, up_taps, gate_bias, up_bias, down_weight
):
    seqs, length, width = tokens.shape
    cb, ra = lax.axis_index("cb"), lax.axis_index("ra")
    core, row, col = cb & 1, ra >> 2, ra & 3
    first = jnp.where(core == 0, col, row)
    second = jnp.where(core == 0, row, col)
    at = jnp.stack([core, first, second]).astype(jnp.int32)
    own_seqs = seqs // 2
    cols = gate_weight.shape[2]
    quarter = cols // 2
    share = quarter // SIDE
    order = (1, 3, 2)

    weights, downs, small = [], [], []
    for l in range(LAYERS):
        own = turn_in(at, gate_weight, up_weight, l)
        weights.append((own, to_twin(own)))
    own = jnp.stack(
        [
            jnp.concatenate([gate_taps, gate_bias[:, None]], axis=1),
            jnp.concatenate([up_taps, up_bias[:, None]], axis=1),
        ]
    )
    coefs = jnp.stack([own, to_twin(own)])
    start = (first & 1) * quarter + second * share
    coefs = lax.dynamic_slice(
        coefs, (first >> 1, 0, 0, 0, start), (1, 2, LAYERS, KERNEL + 1, share)
    )[0]
    small = [coefs[:, l].transpose(0, 2, 1).reshape(2 * share, KERNEL + 1) for l in range(LAYERS)]
    for l in range(LAYERS):
        own = turn_down(at, down_weight, l)
        downs.append((own, to_twin(own)))

    carried, scaled, squares = first_block(at, tokens, norm_gain)
    for l in range(LAYERS):
        own, other = weights[l]
        got = [along_first(piece(at, d, own, other, scaled, squares), d) for d in order]
        got.append(piece(at, 0, own, other, scaled, squares))
        parts = fold(at, got, (*order, 0))
        got = [along_second(part, d) for part, d in zip(parts, order)]
        hidden = gated(at, [*got, parts[3]], small[l], length)

        got = [hidden] + [along_second(hidden, d) for d in (1, 2, 3)]
        block = collected(at, got)
        got = [along_first(block, d) for d in order]
        own, other = downs[l]
        branch = down(at, (0, 1, 3), own, other, [block, got[0], got[1]], None, F32)
        branch = down(at, (2,), own, other, [got[2]], branch, BF16)
        got = [branch] + [along_x(branch, d) for d in (1, 2, 3)]
        if l + 1 < LAYERS:
            carried, scaled, squares = next_block(at, carried, got, norm_gain, l + 1)
    mine = last_block(at, carried, got, own_seqs, length)
    return joined(at, mine, to_twin(mine))


def solution(mesh):
    in_specs = (
        P(None, None, "ra"),
        P(None, "ra"),
        P(None, "ra", "cb"),
        P(None, "ra", "cb"),
        P(None, None, "cb"),
        P(None, None, "cb"),
        P(None, "cb"),
        P(None, "cb"),
        P(None, "cb", "ra"),
    )
    out_specs = P(None, None, "ra")
    return jax.shard_map(
        per_device, mesh=mesh, in_specs=in_specs, out_specs=out_specs, check_vma=False
    )
```

```python
import jax
import jax.numpy as jnp
from jax import lax
from jax.experimental import pallas as pl
from jax.experimental.pallas import tpu as pltpu
from jax.sharding import PartitionSpec as P

D = 4096
KERNEL = 3
LAYERS = 2
SIDE = 4
EXTRA = 16
AXES = ("ra", "cb")
BF16 = jnp.bfloat16
F32 = jnp.float32

eps = 1e-06
resid_scale = 0.5


def pairs(move):
    out = []
    for z in range(SIDE):
        for y in range(SIDE):
            for x in range(SIDE):
                for core in range(2):
                    to_z, to_y, to_x, to_core = move(z, y, x, core)
                    here = ((z * SIDE + y) * SIDE + x) * 2 + core
                    there = ((to_z * SIDE + to_y) * SIDE + to_x) * 2 + to_core
                    out.append((here, there))
    return out


def to_twin(value):
    return lax.ppermute(value, AXES, pairs(lambda z, y, x, c: (z, y, x, 1 - c)))


def along_first(value, d):
    move = lambda z, y, x, c: (z, y ^ d, x, c) if c == 0 else (z ^ d, y, x, c)
    return lax.ppermute(value, AXES, pairs(move))


def along_second(value, d):
    move = lambda z, y, x, c: (z ^ d, y, x, c) if c == 0 else (z, y ^ d, x, c)
    return lax.ppermute(value, AXES, pairs(move))


def along_x(value, d):
    return lax.ppermute(value, AXES, pairs(lambda z, y, x, c: (z, y, x ^ d, c)))


SMEM = pl.BlockSpec(memory_space=pltpu.SMEM)
VMEM = pl.BlockSpec(memory_space=pltpu.VMEM)
HBM = pl.BlockSpec(memory_space=pltpu.HBM)


def local(kernel, name, outs, at, *args, flops=10**9, specs=None, scratch=()):
    many = isinstance(outs, list)
    moved = sum(a.size * a.dtype.itemsize for a in args)
    return pl.pallas_call(
        kernel,
        in_specs=[SMEM] + (specs or [VMEM] * len(args)),
        out_specs=[VMEM] * len(outs) if many else VMEM,
        out_shape=outs,
        scratch_shapes=scratch,
        compiler_params=pltpu.CompilerParams(vmem_limit_bytes=16 * 2**20),
        cost_estimate=pl.CostEstimate(flops=flops, bytes_accessed=moved, transcendentals=0),
        name=name,
    )(at, *args)


def in_hbm(value):
    return pltpu.with_memory_space_constraint(value, pltpu.HBM)


def array(shape, dtype):
    return jax.ShapeDtypeStruct(shape, dtype)


def split_rows(row_sum):
    high = row_sum.astype(BF16).astype(F32)
    low = row_sum - high
    shape = (EXTRA, row_sum.shape[1])
    row = lax.broadcasted_iota(jnp.int32, shape, 0)
    high = jnp.broadcast_to(high, shape)
    low = jnp.broadcast_to(low, shape)
    return jnp.where(row == 0, high, jnp.where(row == 1, low, 0.0)).astype(BF16)


def column(gain, l):
    return jnp.broadcast_to(gain[l : l + 1], (8, gain.shape[1])).T[:, :1]


def store_acts(out, at_row, value, gain_column):
    width = value.shape[0]
    out[at_row : at_row + width] = (value * gain_column).astype(BF16)
    squares = split_rows(jnp.sum(value * value, axis=0, keepdims=True))
    out[at_row + width : at_row + width + EXTRA] = squares


def fetched(refs, l, bufs, sems):
    copies = [pltpu.make_async_copy(r.at[l], b, sems.at[i]) for i, (r, b) in enumerate(zip(refs, bufs))]
    for c in copies:
        c.start()
    return copies


def turned(bufs, turns):
    for buf, turn in zip(bufs, turns):
        turn[...] = buf[...].T


def store_quarter(turns, q, out):
    quarter = turns[0].shape[0] // SIDE
    start = pl.multiple_of(q * quarter, 16)
    for i, turn in enumerate(turns):
        out[i * quarter : (i + 1) * quarter] = turn[pl.ds(start, quarter)]


def turn_scratch(width, cols):
    return [
        pltpu.VMEM((width, cols), BF16),
        pltpu.VMEM((width, cols), BF16),
        pltpu.VMEM((cols, width), BF16),
        pltpu.VMEM((cols, width), BF16),
        pltpu.SemaphoreType.DMA((2,)),
    ]


def first_pack(at, tokens, gain, gate_weight, up_weight, order):
    seqs, length, width = tokens.shape
    cols = gate_weight.shape[2]
    half = seqs // 2 * length
    quarter = cols // 2

    def kernel(at, tokens, gain, gate, up, *refs):
        outs, carried = refs[: len(order)], refs[len(order)]
        bufs, turns, sems = refs[-5:-3], refs[-3:-1], refs[-1]
        copies = fetched((gate, up), 0, bufs, sems)
        gain_column = column(gain, 0)
        for h in range(2):
            mine = tokens[h * (seqs // 2) : (h + 1) * (seqs // 2)].reshape(half, width)
            value = mine.astype(F32).T

            @pl.when(at[0] == h)
            def _():
                carried[...] = value

            for out in outs:
                store_acts(out, quarter + h * (width + EXTRA), value, gain_column)
        for c in copies:
            c.wait()
        turned(bufs, turns)
        for d, out in zip(order, outs):
            store_quarter(turns, at[1] ^ d, out)

    outs = [array((quarter + 2 * (width + EXTRA), width), BF16)] * len(order)
    outs.append(array((width, half), F32))
    return local(
        kernel,
        "first_pack",
        outs,
        at,
        tokens,
        gain,
        in_hbm(gate_weight),
        in_hbm(up_weight),
        specs=[VMEM, VMEM, HBM, HBM],
        scratch=turn_scratch(width, cols),
    )


def turn_in(at, gate_weight, up_weight, l, order):
    _, width, cols = gate_weight.shape

    def kernel(at, gate, up, *refs):
        outs = refs[: len(order)]
        bufs, turns, sems = refs[-5:-3], refs[-3:-1], refs[-1]
        for c in fetched((gate, up), l, bufs, sems):
            c.wait()
        turned(bufs, turns)
        for d, out in zip(order, outs):
            store_quarter(turns, at[1] ^ d, out)

    return local(
        kernel,
        "turn_in",
        [array((cols // 2, width), BF16)] * len(order),
        at,
        in_hbm(gate_weight),
        in_hbm(up_weight),
        specs=[HBM, HBM],
        scratch=turn_scratch(width, cols),
    )


def turn_down(at, down_weight, l):
    _, cols, width = down_weight.shape
    quarter = cols // SIDE

    def kernel(at, weights, out, buf, sems):
        for c in fetched((weights,), l, (buf,), sems):
            c.wait()
        for q in range(SIDE):
            out[q] = buf[q * quarter : (q + 1) * quarter].T

    return local(
        kernel,
        "turn_down",
        array((SIDE, width, quarter), BF16),
        at,
        in_hbm(down_weight),
        specs=[HBM],
        scratch=[pltpu.VMEM((cols, width), BF16), pltpu.SemaphoreType.DMA((1,))],
    )


def added(carried, parts):
    a, b, c, d = (p[...].astype(F32) for p in parts)
    return resid_scale * carried[...] + ((a + b) + (c + d))


def next_block(at, carried, parts, gain, l):
    def kernel(at, carried, a, b, c, d, gain, out, acts):
        value = added(carried, (a, b, c, d))
        out[...] = value
        store_acts(acts, 0, value, column(gain, l))

    width, rows = carried.shape
    outs = [array((width, rows), F32), array((width + EXTRA, rows), BF16)]
    return local(kernel, "next_block", outs, at, carried, *parts, gain)


def last_block(at, carried, parts, seqs, length):
    def kernel(at, carried, a, b, c, d, out):
        out[...] = added(carried, (a, b, c, d)).T.astype(BF16).reshape(out.shape)

    out = array((seqs, length, carried.shape[0]), BF16)
    return local(kernel, "last_block", out, at, carried, *parts)


def joined(at, mine, other):
    seqs, length, width = mine.shape

    def kernel(at, mine, other, out):
        out[pl.ds(at[0] * seqs, seqs)] = mine[...]
        out[pl.ds((1 - at[0]) * seqs, seqs)] = other[...]

    return local(kernel, "joined", array((2 * seqs, length, width), BF16), at, mine, other)


def products(at, shape, rows, operands, read, order):
    quarter, width = shape
    share = quarter // (2 * SIDE)

    def kernel(at, *refs):
        ins, outs, acc = refs[: len(operands)], refs[len(operands) : -1], refs[-1]
        half = rows // 2
        for h in range(2):
            total, squares = 0.0, 0.0
            for weights, acts, extra in read(ins, h, at):
                total = total + jnp.dot(weights, acts, preferred_element_type=F32)
                extra = extra.astype(F32)
                squares = squares + extra[0:1] + extra[1:2]
            acc[:, h * half : (h + 1) * half] = total
            squares = split_rows(squares)
            for out in outs:
                out[2 * share :, h * half : (h + 1) * half] = squares
        for d, out in zip(order, outs):
            start = pl.multiple_of((at[2] ^ d) * share, 8)
            gate = acc[pl.ds(start, share)]
            up = acc[pl.ds(start + quarter // 2, share)]
            out[: 2 * share] = jnp.concatenate([gate, up], axis=0).astype(BF16)

    return local(
        kernel,
        "products",
        [array((2 * share + EXTRA, rows), BF16)] * len(order),
        at,
        *operands,
        flops=2 * quarter * SIDE * width * rows,
        scratch=[pltpu.VMEM((quarter, rows), F32)],
    )


def first_products(at, packs, quarter, width, rows, order):
    def read(refs, h, at):
        start = quarter + h * (width + EXTRA)
        for ref in refs:
            acts = ref[start : start + width]
            yield ref[:quarter], acts, ref[start + width : start + width + EXTRA]

    return products(at, (quarter, width), rows, packs, read, order)


def halves(at, mine, other):
    count = mine.shape[0]

    def kernel(at, mine, other, out):
        for h in range(2):

            @pl.when(at[0] == h)
            def _():
                out[h * count : (h + 1) * count] = mine[...]
                out[(1 - h) * count : (2 - h) * count] = other[...]

    return local(kernel, "halves", array((2 * count, mine.shape[1]), mine.dtype), at, mine, other)


def next_products(at, weights, acts, width, rows, order):
    quarter = weights[0].shape[0]
    n = len(weights)

    def read(refs, h, at):
        start = h * (width + EXTRA)
        for w, a in zip(refs[:n], refs[n:]):
            yield w[...], a[start : start + width], a[start + width : start + width + EXTRA]

    return products(at, (quarter, width), rows, [*weights, *acts], read, order)


def gated(at, parts, small, length):
    total, rows = parts[0].shape
    share = (total - EXTRA) // 2

    def kernel(at, a, b, c, d, small, out):
        coef = small[...]
        lane = lax.broadcasted_iota(jnp.int32, (2 * share, length), 1)
        for s in range(rows // length):
            cut = slice(s * length, (s + 1) * length)
            a_, b_, c_, d_ = (p[:, cut].astype(F32) for p in (a, b, c, d))
            value = (a_ + b_) + (c_ + d_)
            row_squares = value[2 * share : 2 * share + 1] + value[2 * share + 1 : 2 * share + 2]
            inverse = lax.rsqrt(row_squares / D + eps)
            now = (value[: 2 * share] * inverse).astype(BF16).astype(F32)
            one = jnp.where(lane >= 1, pltpu.roll(now, 1, 1), 0.0)
            two = jnp.where(lane >= 2, pltpu.roll(now, 2, 1), 0.0)
            conv = coef[:, 3:4] + coef[:, 0:1] * two + coef[:, 1:2] * one + coef[:, 2:3] * now
            gate, up = conv[:share], conv[share:]
            result = gate / (1.0 + jnp.exp(-gate)) * up
            out[:, cut] = result.astype(BF16)

    return local(kernel, "gated", array((share, rows), BF16), at, *parts, small)


def collected(at, parts, ds):
    share, rows = parts[0].shape

    def kernel(at, *refs):
        out, buf = refs[SIDE], refs[SIDE + 1]
        for d, ref in zip(ds, refs):
            start = pl.multiple_of((at[2] ^ d) * share, 8)
            buf[pl.ds(start, share)] = ref[...].astype(F32)
        out[...] = buf[...].astype(BF16)

    out = array((SIDE * share, rows), BF16)
    scratch = [pltpu.VMEM((SIDE * share, rows), F32)]
    return local(kernel, "collected", out, at, *parts, scratch=scratch)


def down(at, ds, weights, blocks, carry):
    _, width, quarter = weights.shape
    n, half = len(blocks), blocks[0].shape[1] // 2
    carries = [] if carry is None else list(carry)

    def kernel(at, weights, *refs):
        blocks, rest = refs[:n], refs[n:]
        for h in range(2):
            out = rest[-2 + h]
            cut = pl.ds(pl.multiple_of((at[0] ^ h) * half, 128), half)
            total = rest[h][...] if carries else 0.0
            for d, block in zip(ds, blocks):
                total = total + jnp.dot(
                    weights[at[1] ^ d], block[:, cut], preferred_element_type=F32
                )
            out[...] = total.astype(out.dtype)

    flops = 4 * n * width * quarter * half
    outs = [array((width, half), F32), array((width, half), BF16 if carries else F32)]
    return local(kernel, "down", outs, at, weights, *blocks, *carries, flops=flops)


def paired(at, mine, other):
    def kernel(at, mine, other, out):
        out[...] = (mine[...] + other[...].astype(F32)).astype(BF16)

    return local(kernel, "paired", array(mine.shape, BF16), at, mine, other)


def after(values, *earlier):
    return lax.optimization_barrier((values, *earlier))[0]


def per_device(
    tokens, norm_gain, gate_weight, up_weight, gate_taps, up_taps, gate_bias, up_bias, down_weight
):
    seqs, length, width = tokens.shape
    rows = seqs * length
    cb, ra = lax.axis_index("cb"), lax.axis_index("ra")
    core, row, col = cb & 1, ra >> 2, ra & 3
    first = jnp.where(core == 0, col, row)
    second = jnp.where(core == 0, row, col)
    at = jnp.stack([core, first, second]).astype(jnp.int32)
    cols = gate_weight.shape[2]
    share = cols // (SIDE * SIDE)
    order = (1, 3, 2)
    every = (*order, 0)

    coefs = jnp.stack(
        [
            jnp.concatenate([gate_taps, gate_bias[:, None]], axis=1),
            jnp.concatenate([up_taps, up_bias[:, None]], axis=1),
        ]
    )
    coefs = lax.dynamic_slice_in_dim(coefs, (first * SIDE + second) * share, share, 3)
    small = [coefs[:, l].transpose(0, 2, 1).reshape(2 * share, KERNEL + 1) for l in range(LAYERS)]

    tokens = after(tokens, *small)
    *packs, carried = first_pack(at, tokens, norm_gain, gate_weight, up_weight, every)
    turned = turn_in(at, gate_weight, up_weight, 1, every)
    downs = [turn_down(at, down_weight, l) for l in range(LAYERS)]
    packs = [along_first(p, d) for p, d in zip(packs, order)] + [packs[3]]
    packs = after(packs, *downs, turned[3])
    parts = first_products(at, packs, cols // 2, width, rows, every)
    for l in range(LAYERS):
        more = l + 1 < LAYERS
        got = [along_second(part, d) for part, d in zip(parts, order)]
        if more:
            weights = [along_first(after(turned[0], *parts), order[0])]
        hidden = gated(at, [*got, parts[3]], small[l], length)
        if more:
            weights.append(along_first(after(turned[1], hidden), order[1]))
        got = [along_second(hidden, d) for d in order]
        if more:
            got, weights[0] = lax.optimization_barrier((got, weights[0]))
        block = collected(at, [*got, hidden], every)
        if more:
            weights.append(along_first(after(turned[2], block), order[2]))
            weights.append(turned[3])
        got = [along_first(block, d) for d in order]
        if more:
            got, weights[1] = lax.optimization_barrier((got, weights[1]))
        branch = down(at, (0, 1, 3), downs[l], [block, got[0], got[1]], None)
        mine, twins = down(at, (2,), downs[l], [got[2]], branch)
        twins = to_twin(twins)
        if more:
            twins, weights[2] = lax.optimization_barrier((twins, weights[2]))
        branch = paired(at, mine, twins)
        got = [branch] + [along_x(branch, d) for d in (1, 2, 3)]
        if more:
            carried, acts = next_block(at, carried, got, norm_gain, l + 1)
            acts = halves(at, acts, to_twin(acts))
            acts = [along_first(acts, d) for d in order] + [acts]
            parts = next_products(at, weights, acts, width, rows, every)
    mine = last_block(at, carried, got, seqs // 2, length)
    return joined(at, mine, to_twin(mine))


def solution(mesh):
    in_specs = (
        P(None, None, "ra"),
        P(None, "ra"),
        P(None, "ra", "cb"),
        P(None, "ra", "cb"),
        P(None, None, "cb"),
        P(None, None, "cb"),
        P(None, "cb"),
        P(None, "cb"),
        P(None, "cb", "ra"),
    )
    out_specs = P(None, None, "ra")
    return jax.shard_map(
        per_device, mesh=mesh, in_specs=in_specs, out_specs=out_specs, check_vma=False
    )
```

```python
import jax
import jax.numpy as jnp
from jax import lax
from jax.experimental import pallas as pl
from jax.experimental.pallas import tpu as pltpu
from jax.sharding import PartitionSpec as P

D = 4096
KERNEL = 3
LAYERS = 2
SIDE = 4
EXTRA = 16
AXES = ("ra", "cb")
BF16 = jnp.bfloat16
F32 = jnp.float32

eps = 1e-06
resid_scale = 0.5


def pairs(move):
    out = []
    for z in range(SIDE):
        for y in range(SIDE):
            for x in range(SIDE):
                for core in range(2):
                    to_z, to_y, to_x, to_core = move(z, y, x, core)
                    here = ((z * SIDE + y) * SIDE + x) * 2 + core
                    there = ((to_z * SIDE + to_y) * SIDE + to_x) * 2 + to_core
                    out.append((here, there))
    return out


def to_twin(value):
    return lax.ppermute(value, AXES, pairs(lambda z, y, x, c: (z, y, x, 1 - c)))


def along_first(value, d):
    move = lambda z, y, x, c: (z, y ^ d, x, c) if c == 0 else (z ^ d, y, x, c)
    return lax.ppermute(value, AXES, pairs(move))


def along_second(value, d):
    move = lambda z, y, x, c: (z ^ d, y, x, c) if c == 0 else (z, y ^ d, x, c)
    return lax.ppermute(value, AXES, pairs(move))


def along_x(value, d):
    return lax.ppermute(value, AXES, pairs(lambda z, y, x, c: (z, y, x ^ d, c)))


VMEM = pl.BlockSpec(memory_space=pltpu.VMEM)
HBM = pl.BlockSpec(memory_space=pltpu.HBM)


def position():
    cb, ra = lax.axis_index("cb"), lax.axis_index("ra")
    core, row, col = cb & 1, ra >> 2, ra & 3
    return core, jnp.where(core == 0, col, row), jnp.where(core == 0, row, col)


def local(kernel, name, outs, *args, flops=10**9, specs=None, scratch=()):
    many = isinstance(outs, list)
    moved = sum(a.size * a.dtype.itemsize for a in args)
    return pl.pallas_call(
        kernel,
        in_specs=specs or [VMEM] * len(args),
        out_specs=[VMEM] * len(outs) if many else VMEM,
        out_shape=outs,
        scratch_shapes=scratch,
        compiler_params=pltpu.CompilerParams(vmem_limit_bytes=16 * 2**20),
        cost_estimate=pl.CostEstimate(flops=flops, bytes_accessed=moved, transcendentals=0),
        name=name,
    )(*args)


def in_hbm(value):
    return pltpu.with_memory_space_constraint(value, pltpu.HBM)


def array(shape, dtype):
    return jax.ShapeDtypeStruct(shape, dtype)


def split_rows(row_sum):
    high = row_sum.astype(BF16).astype(F32)
    low = row_sum - high
    shape = (EXTRA, row_sum.shape[1])
    row = lax.broadcasted_iota(jnp.int32, shape, 0)
    high = jnp.broadcast_to(high, shape)
    low = jnp.broadcast_to(low, shape)
    return jnp.where(row == 0, high, jnp.where(row == 1, low, 0.0)).astype(BF16)


def column(gain, l):
    return jnp.broadcast_to(gain[l : l + 1], (8, gain.shape[1])).T[:, :1]


def store_acts(out, at_row, value, gain_column):
    width = value.shape[0]
    out[at_row : at_row + width] = (value * gain_column).astype(BF16)
    squares = split_rows(jnp.sum(value * value, axis=0, keepdims=True))
    out[at_row + width : at_row + width + EXTRA] = squares


def fetched(refs, bufs, sems):
    copies = [pltpu.make_async_copy(r, b, sems.at[i]) for i, (r, b) in enumerate(zip(refs, bufs))]
    for c in copies:
        c.start()
    return copies


def store_quarter(turns, q, out):
    quarter = turns[0].shape[0] // SIDE
    start = pl.multiple_of(q * quarter, 16)
    for i, turn in enumerate(turns):
        out[i * quarter : (i + 1) * quarter] = turn[pl.ds(start, quarter)]


def turn_scratch(width, cols):
    return [
        pltpu.VMEM((width, cols), BF16),
        pltpu.VMEM((width, cols), BF16),
        pltpu.VMEM((cols, width), BF16),
        pltpu.VMEM((cols, width), BF16),
    ]


def first_pack(tokens, gain, gate_weight, up_weight, order):
    seqs, length, width = tokens.shape
    cols = gate_weight.shape[2]
    half = seqs // 2 * length
    quarter = cols // 2
    n = len(order)

    def kernel(tokens, gain, gate, up, *refs):
        outs, carried = refs[:n], refs[n]
        gate_buf, up_buf, *turns, token_buf, gain_buf, sems = refs[n + 1 :]
        core, first, _ = position()
        copies = fetched(
            (tokens, gain, gate.at[0], up.at[0]), (token_buf, gain_buf, gate_buf, up_buf), sems
        )
        copies[0].wait()
        copies[1].wait()
        gain_column = column(gain_buf, 0)
        for h in range(2):
            place = core ^ h
            mine = token_buf[pl.ds(place * (seqs // 2), seqs // 2)].reshape(half, width)
            value = mine.astype(F32).T
            if h == 0:
                carried[...] = value
            for out in outs:
                store_acts(out, quarter + h * (width + EXTRA), value, gain_column)
        for c, buf, turn in zip(copies[2:], (gate_buf, up_buf), turns):
            c.wait()
            turn[...] = buf[...].T
        for d, out in zip(order, outs):
            store_quarter(turns, first ^ d, out)

    outs = [array((quarter + 2 * (width + EXTRA), width), BF16)] * n
    outs.append(array((width, half), F32))
    return local(
        kernel,
        "first_pack",
        outs,
        *map(in_hbm, (tokens, gain, gate_weight, up_weight)),
        specs=[HBM] * 4,
        scratch=[
            *turn_scratch(width, cols),
            pltpu.VMEM(tokens.shape, BF16),
            pltpu.VMEM(gain.shape, F32),
            pltpu.SemaphoreType.DMA((4,)),
        ],
    )


def turn_in(gate_weight, up_weight, l, order):
    _, width, cols = gate_weight.shape
    n = len(order)

    def kernel(gate, up, *refs):
        outs = refs[:n]
        gate_buf, up_buf, *turns, sems = refs[n:]
        _, first, _ = position()
        copies = fetched((gate.at[l], up.at[l]), (gate_buf, up_buf), sems)
        for c, buf, turn in zip(copies, (gate_buf, up_buf), turns):
            c.wait()
            turn[...] = buf[...].T
        for d, out in zip(order, outs):
            store_quarter(turns, first ^ d, out)

    return local(
        kernel,
        "turn_in",
        [array((cols // 2, width), BF16)] * n,
        *map(in_hbm, (gate_weight, up_weight)),
        specs=[HBM, HBM],
        scratch=[*turn_scratch(width, cols), pltpu.SemaphoreType.DMA((2,))],
    )


def turn_down(down_weight, l):
    _, cols, width = down_weight.shape
    quarter = cols // SIDE

    def kernel(weights, out, buf, sems):
        for c in fetched((weights.at[l],), (buf,), sems):
            c.wait()
        for q in range(SIDE):
            out[q] = buf[q * quarter : (q + 1) * quarter].T

    return local(
        kernel,
        "turn_down",
        array((SIDE, width, quarter), BF16),
        in_hbm(down_weight),
        specs=[HBM],
        scratch=[pltpu.VMEM((cols, width), BF16), pltpu.SemaphoreType.DMA((1,))],
    )


def turn_small(gate_taps, up_taps, gate_bias, up_bias):
    layers, cols = gate_bias.shape
    share = cols // (SIDE * SIDE)
    lanes = 128

    def kernel(gate_taps, up_taps, gate_bias, up_bias, out):
        _, first, second = position()
        start = (first * SIDE + second) * share
        for l in range(layers):
            rows = []
            for taps, bias in ((gate_taps, gate_bias), (up_taps, up_bias)):
                rows += [taps[t, l : l + 1] for t in range(KERNEL)] + [bias[l : l + 1]]
            rows = jnp.concatenate(rows, axis=0)
            rows = pltpu.roll(rows, lax.rem(cols - start, cols), 1)
            out[l] = rows[:, :lanes].T

    turn = lambda taps: jnp.transpose(taps, (1, 0, 2))
    out = array((layers, lanes, 2 * (KERNEL + 1)), F32)
    return local(kernel, "turn_small", out, turn(gate_taps), turn(up_taps), gate_bias, up_bias)


def added(carried, parts):
    a, b, c, d = (p[...].astype(F32) for p in parts)
    return resid_scale * carried[...] + ((a + b) + (c + d))


def next_block(carried, parts, gain, l):
    def kernel(carried, a, b, c, d, gain, out, acts):
        value = added(carried, (a, b, c, d))
        out[...] = value
        store_acts(acts, 0, value, column(gain, l))

    width, rows = carried.shape
    outs = [array((width, rows), F32), array((width + EXTRA, rows), BF16)]
    return local(kernel, "next_block", outs, carried, *parts, gain)


def last_block(carried, parts, seqs, length):
    def kernel(carried, a, b, c, d, out):
        out[...] = added(carried, (a, b, c, d)).T.astype(BF16).reshape(out.shape)

    out = array((seqs, length, carried.shape[0]), BF16)
    return local(kernel, "last_block", out, carried, *parts)


def joined(mine, other):
    seqs, length, width = mine.shape

    def kernel(mine, other, out):
        core, _, _ = position()
        out[pl.ds(core * seqs, seqs)] = mine[...]
        out[pl.ds((1 - core) * seqs, seqs)] = other[...]

    return local(kernel, "joined", array((2 * seqs, length, width), BF16), mine, other)


def stacked(mine, other):
    count = mine.shape[0]

    def kernel(mine, other, out):
        out[:count] = mine[...]
        out[count:] = other[...]

    return local(kernel, "stacked", array((2 * count, mine.shape[1]), mine.dtype), mine, other)


def products(quarter, width, half, operands, read, order):
    share = quarter // (2 * SIDE)

    def kernel(*refs):
        ins, outs, acc = refs[: len(operands)], refs[len(operands) : -1], refs[-1]
        _, _, second = position()
        for h in range(2):
            total, squares = 0.0, 0.0
            for weights, acts, extra in read(ins, h):
                total = total + jnp.dot(weights, acts, preferred_element_type=F32)
                extra = extra.astype(F32)
                squares = squares + extra[0:1] + extra[1:2]
            acc[:, h * half : (h + 1) * half] = total
            squares = split_rows(squares)
            for out in outs:
                out[2 * share :, h * half : (h + 1) * half] = squares
        for d, out in zip(order, outs):
            start = pl.multiple_of((second ^ d) * share, 8)
            gate = acc[pl.ds(start, share)]
            up = acc[pl.ds(start + quarter // 2, share)]
            out[: 2 * share] = jnp.concatenate([gate, up], axis=0).astype(BF16)

    return local(
        kernel,
        "products",
        [array((2 * share + EXTRA, 2 * half), BF16)] * len(order),
        *operands,
        flops=4 * quarter * SIDE * width * half,
        scratch=[pltpu.VMEM((quarter, 2 * half), F32)],
    )


def first_products(packs, quarter, width, half, order):
    def read(refs, h):
        start = quarter + h * (width + EXTRA)
        for ref in refs:
            acts = ref[start : start + width]
            yield ref[:quarter], acts, ref[start + width : start + width + EXTRA]

    return products(quarter, width, half, packs, read, order)


def next_products(weights, acts, width, half, order):
    n = len(weights)

    def read(refs, h):
        start = h * (width + EXTRA)
        for w, a in zip(refs[:n], refs[n:]):
            yield w[...], a[start : start + width], a[start + width : start + width + EXTRA]

    return products(weights[0].shape[0], width, half, [*weights, *acts], read, order)


def gated(parts, small, l, length):
    total, rows = parts[0].shape
    share = (total - EXTRA) // 2

    def kernel(a, b, c, d, small, out):
        coef = small[l, :share]
        lane = lax.broadcasted_iota(jnp.int32, (share, length), 1)

        def conv(now, k):
            one = jnp.where(lane >= 1, pltpu.roll(now, 1, 1), 0.0)
            two = jnp.where(lane >= 2, pltpu.roll(now, 2, 1), 0.0)
            early = coef[:, k + 3 : k + 4] + coef[:, k : k + 1] * two
            return early + coef[:, k + 1 : k + 2] * one + coef[:, k + 2 : k + 3] * now

        for s in range(rows // length):
            cut = slice(s * length, (s + 1) * length)
            a_, b_, c_, d_ = (p[:, cut].astype(F32) for p in (a, b, c, d))
            value = (a_ + b_) + (c_ + d_)
            row_squares = value[2 * share : 2 * share + 1] + value[2 * share + 1 : 2 * share + 2]
            inverse = lax.rsqrt(row_squares / D + eps)
            now = (value[: 2 * share] * inverse).astype(BF16).astype(F32)
            gate, up = conv(now[:share], 0), conv(now[share:], KERNEL + 1)
            result = gate / (1.0 + jnp.exp(-gate)) * up
            out[:, cut] = result.astype(BF16)

    return local(kernel, "gated", array((share, rows), BF16), *parts, small)


def collected(parts, ds):
    share, rows = parts[0].shape

    def kernel(*refs):
        out, buf = refs[SIDE], refs[SIDE + 1]
        _, _, second = position()
        for d, ref in zip(ds, refs):
            start = pl.multiple_of((second ^ d) * share, 8)
            buf[pl.ds(start, share)] = ref[...].astype(F32)
        out[...] = buf[...].astype(BF16)

    out = array((SIDE * share, rows), BF16)
    scratch = [pltpu.VMEM((SIDE * share, rows), F32)]
    return local(kernel, "collected", out, *parts, scratch=scratch)


def down(ds, weights, blocks, carry):
    _, width, quarter = weights.shape
    n, half = len(blocks), blocks[0].shape[1] // 2
    carries = [] if carry is None else list(carry)

    def kernel(weights, *refs):
        blocks, rest = refs[:n], refs[n:]
        _, first, _ = position()
        for h in range(2):
            out = rest[-2 + h]
            total = rest[h][...] if carries else 0.0
            for d, block in zip(ds, blocks):
                total = total + jnp.dot(
                    weights[first ^ d],
                    block[:, h * half : (h + 1) * half],
                    preferred_element_type=F32,
                )
            out[...] = total.astype(out.dtype)

    flops = 4 * n * width * quarter * half
    outs = [array((width, half), F32), array((width, half), BF16 if carries else F32)]
    return local(kernel, "down", outs, weights, *blocks, *carries, flops=flops)


def paired(mine, other):
    def kernel(mine, other, out):
        out[...] = (mine[...] + other[...].astype(F32)).astype(BF16)

    return local(kernel, "paired", array(mine.shape, BF16), mine, other)


def after(values, *earlier):
    return lax.optimization_barrier((values, *earlier))[0]


def per_device(
    tokens, norm_gain, gate_weight, up_weight, gate_taps, up_taps, gate_bias, up_bias, down_weight
):
    seqs, length, width = tokens.shape
    half = seqs // 2 * length
    quarter = gate_weight.shape[2] // 2
    order = (1, 3, 2)
    every = (*order, 0)

    *packs, carried = first_pack(tokens, norm_gain, gate_weight, up_weight, every)
    turned = turn_in(gate_weight, up_weight, 1, every)
    downs = [turn_down(down_weight, l) for l in range(LAYERS)]
    small = turn_small(gate_taps, up_taps, gate_bias, up_bias)
    packs = [along_first(p, d) for p, d in zip(packs, order)] + [packs[3]]
    packs = after(packs, *downs, turned[3], small)
    parts = first_products(packs, quarter, width, half, every)
    for l in range(LAYERS):
        more = l + 1 < LAYERS
        got = [along_second(part, d) for part, d in zip(parts, order)]
        hidden = gated([*got, parts[3]], small, l, length)
        got = [along_second(hidden, d) for d in order]
        block = collected([*got, hidden], every)
        got = [along_first(block, d) for d in order]
        branch = down((0, 1, 3), downs[l], [block, got[0], got[1]], None)
        mine, twins = down((2,), downs[l], [got[2]], branch)
        if more:
            weights = [along_first(after(turned[0], twins), order[0])]
        branch = paired(mine, to_twin(twins))
        got = [branch] + [along_x(branch, d) for d in (1, 2, 3)]
        if more:
            weights += [along_first(after(t, branch), d) for t, d in zip(turned[1:], order[1:])]
            got, weights = lax.optimization_barrier((got, weights))
            weights.append(turned[3])
            carried, acts = next_block(carried, got, norm_gain, l + 1)
            acts = stacked(acts, to_twin(acts))
            acts = [along_first(acts, d) for d in order] + [acts]
            parts = next_products(weights, acts, width, half, every)
    mine = last_block(carried, got, seqs // 2, length)
    return joined(mine, to_twin(mine))


def solution(mesh):
    in_specs = (
        P(None, None, "ra"),
        P(None, "ra"),
        P(None, "ra", "cb"),
        P(None, "ra", "cb"),
        P(None, None, "cb"),
        P(None, None, "cb"),
        P(None, "cb"),
        P(None, "cb"),
        P(None, "cb", "ra"),
    )
    out_specs = P(None, None, "ra")
    return jax.shard_map(
        per_device, mesh=mesh, in_specs=in_specs, out_specs=out_specs, check_vma=False
    )
```

```python
import jax
import jax.numpy as jnp
from jax import lax
from jax.experimental import pallas as pl
from jax.experimental.pallas import tpu as pltpu
from jax.sharding import PartitionSpec as P


D = 4096
KERNEL = 3
LAYERS = 2
SIDE = 4
EXTRA = 16
AXES = ("ra", "cb")
BF16 = jnp.bfloat16
F32 = jnp.float32

eps = 1e-06
resid_scale = 0.5


def pairs(move):
    out = []
    for z in range(SIDE):
        for y in range(SIDE):
            for x in range(SIDE):
                for core in range(2):
                    to_z, to_y, to_x, to_core = move(z, y, x, core)
                    here = ((z * SIDE + y) * SIDE + x) * 2 + core
                    there = ((to_z * SIDE + to_y) * SIDE + to_x) * 2 + to_core
                    out.append((here, there))
    return out


def to_twin(value):
    return lax.ppermute(value, AXES, pairs(lambda z, y, x, c: (z, y, x, 1 - c)))


def first_move(d):
    return lambda z, y, x, c: (z, y ^ d, x, c) if c == 1 else (z ^ d, y, x, c)


def second_move(d):
    return lambda z, y, x, c: (z ^ d, y, x, c) if c == 1 else (z, y ^ d, x, c)


def x_move(d):
    return lambda z, y, x, c: (z, y, x ^ d, c)


def moved(move, values):
    got = {}
    for d in (1, 2, 3):
        got[d] = lax.ppermute(values[d], AXES, pairs(move(d)))
    return got


VMEM = pl.BlockSpec(memory_space=pltpu.VMEM)
HBM = pl.BlockSpec(memory_space=pltpu.HBM)


def position():
    cb, ra = lax.axis_index("cb"), lax.axis_index("ra")
    core, row, col = cb & 1, ra >> 2, ra & 3
    return core, jnp.where(core == 1, col, row), jnp.where(core == 1, row, col)


def local(kernel, outs, *args, flops=10**9, specs=None, scratch=()):
    many = isinstance(outs, list)
    moved = sum(a.size * a.dtype.itemsize for a in args)
    return pl.pallas_call(
        kernel,
        in_specs=specs or [VMEM] * len(args),
        out_specs=[VMEM] * len(outs) if many else VMEM,
        out_shape=outs,
        scratch_shapes=scratch,
        compiler_params=pltpu.CompilerParams(vmem_limit_bytes=16 * 2**20),
        cost_estimate=pl.CostEstimate(flops=flops, bytes_accessed=moved, transcendentals=0),
    )(*args)


def in_hbm(value):
    return pltpu.with_memory_space_constraint(value, pltpu.HBM)


def array(shape, dtype):
    return jax.ShapeDtypeStruct(shape, dtype)


def split_rows(row_sum):
    high = row_sum.astype(BF16).astype(F32)
    low = row_sum - high
    shape = (EXTRA, row_sum.shape[1])
    row = lax.broadcasted_iota(jnp.int32, shape, 0)
    high = jnp.broadcast_to(high, shape)
    low = jnp.broadcast_to(low, shape)
    return jnp.where(row == 0, high, jnp.where(row == 1, low, 0.0)).astype(BF16)


def column(gain, l):
    return jnp.broadcast_to(gain[l : l + 1], (8, gain.shape[1])).T[:, :1]


def store_acts(out, at_row, value, gain_column):
    width = value.shape[0]
    out[at_row : at_row + width] = (value * gain_column).astype(BF16)
    squares = split_rows(jnp.sum(value * value, axis=0, keepdims=True))
    out[at_row + width : at_row + width + EXTRA] = squares


def fetched(refs, bufs, sems):
    copies = [pltpu.make_async_copy(r, b, sems.at[i]) for i, (r, b) in enumerate(zip(refs, bufs))]
    for c in copies:
        c.start()
    return copies


def store_quarter(turns, q, out):
    quarter = turns[0].shape[0] // SIDE
    start = pl.multiple_of(q * quarter, 16)
    for i, turn in enumerate(turns):
        out[i * quarter : (i + 1) * quarter] = turn[pl.ds(start, quarter)]


def turn_scratch(width, cols):
    return [
        pltpu.VMEM((width, cols), BF16),
        pltpu.VMEM((width, cols), BF16),
        pltpu.VMEM((cols, width), BF16),
        pltpu.VMEM((cols, width), BF16),
    ]


def first_pack(tokens, gain, gate_weight, up_weight, order):
    seqs, length, width = tokens.shape
    cols = gate_weight.shape[2]
    half = seqs // 2 * length
    quarter = cols // 2
    n = len(order)

    def kernel(tokens, gain, gate, up, *refs):
        outs, carried = refs[:n], refs[n]
        gate_buf, up_buf, *turns, token_buf, gain_buf, sems = refs[n + 1 :]
        core, first, _ = position()
        copies = fetched(
            (tokens, gain, gate.at[0], up.at[0]), (token_buf, gain_buf, gate_buf, up_buf), sems
        )
        copies[0].wait()
        copies[1].wait()
        gain_column = column(gain_buf, 0)
        for h in range(2):
            place = core ^ h
            mine = token_buf[pl.ds(place * (seqs // 2), seqs // 2)].reshape(half, width)
            value = mine.astype(F32).T
            if h == 0:
                carried[...] = value
            for out in outs:
                store_acts(out, quarter + h * (width + EXTRA), value, gain_column)
        for c, buf, turn in zip(copies[2:], (gate_buf, up_buf), turns):
            c.wait()
            turn[...] = buf[...].T
        for d, out in zip(order, outs):
            store_quarter(turns, first ^ d, out)

    outs = [array((quarter + 2 * (width + EXTRA), width), BF16)] * n
    outs.append(array((width, half), F32))
    return local(
        kernel,
        outs,
        *map(in_hbm, (tokens, gain, gate_weight, up_weight)),
        specs=[HBM] * 4,
        scratch=[
            *turn_scratch(width, cols),
            pltpu.VMEM(tokens.shape, BF16),
            pltpu.VMEM(gain.shape, F32),
            pltpu.SemaphoreType.DMA((4,)),
        ],
    )


def turn_in(gate_weight, up_weight, l):
    _, width, cols = gate_weight.shape
    quarter = cols // 2

    def kernel(gate, up, out, gate_buf, up_buf, *rest):
        *turns, sems = rest
        copies = fetched((gate.at[l], up.at[l]), (gate_buf, up_buf), sems)
        for c, buf, turn in zip(copies, (gate_buf, up_buf), turns):
            c.wait()
            turn[...] = buf[...].T
        for q in range(SIDE):
            store_quarter(turns, q, out.at[q * quarter : (q + 1) * quarter])

    return local(
        kernel,
        array((SIDE * quarter, width), BF16),
        *map(in_hbm, (gate_weight, up_weight)),
        specs=[HBM, HBM],
        scratch=[*turn_scratch(width, cols), pltpu.SemaphoreType.DMA((2,))],
    )


def mixed(mine, twins, order):
    rows, width = mine.shape
    quarter = rows // SIDE

    def kernel(mine, twins, *outs):
        _, first, _ = position()
        for d, out in zip(order, outs):
            start = pl.multiple_of((first ^ d) * quarter, 16)
            out[:quarter] = mine[pl.ds(start, quarter)]
            out[quarter:] = twins[pl.ds(start, quarter)]

    return local(kernel, [array((2 * quarter, width), BF16)] * len(order), mine, twins)


def turn_down(down_weight, l):
    _, cols, width = down_weight.shape
    quarter = cols // SIDE

    def kernel(weights, out, buf, sems):
        for c in fetched((weights.at[l],), (buf,), sems):
            c.wait()
        for q in range(SIDE):
            out[q, :, :quarter] = buf[q * quarter : (q + 1) * quarter].T

    return local(
        kernel,
        array((SIDE, width, pl.cdiv(quarter, 128) * 128), BF16),
        in_hbm(down_weight),
        specs=[HBM],
        scratch=[pltpu.VMEM((cols, width), BF16), pltpu.SemaphoreType.DMA((1,))],
    )


def pack_small(gate_taps, up_taps, gate_bias, up_bias):
    layers, cols = gate_bias.shape

    def kernel(gate_taps, up_taps, gate_bias, up_bias, out):
        for l in range(layers):
            rows = []
            for taps, bias in ((gate_taps, gate_bias), (up_taps, up_bias)):
                rows += [taps[t, l : l + 1] for t in range(KERNEL)] + [bias[l : l + 1]]
            out[l] = jnp.concatenate(rows, axis=0)

    turn = lambda taps: jnp.transpose(taps, (1, 0, 2))
    out = array((layers, 2 * (KERNEL + 1), cols), F32)
    return local(kernel, out, turn(gate_taps), turn(up_taps), gate_bias, up_bias)


def turn_small(mine, twins):
    layers, count, cols = mine.shape
    share = cols // (SIDE * SIDE)
    lanes = 128

    def kernel(mine, twins, out):
        _, first, second = position()
        shift = lax.rem(cols - (first * SIDE + second) * share, cols)
        for i, ref in enumerate((mine, twins)):
            for l in range(layers):
                out[i * layers + l] = pltpu.roll(ref[l], shift, 1)[:, :lanes].T

    return local(kernel, array((2 * layers, lanes, count), F32), mine, twins)


def added(carried, parts):
    a, b, c, d = (p[...].astype(F32) for p in parts)
    return resid_scale * carried[...] + ((a + b) + (c + d))


def next_block(carried, parts, gain, l):
    def kernel(carried, a, b, c, d, gain, out, acts):
        value = added(carried, (a, b, c, d))
        out[...] = value
        store_acts(acts, 0, value, column(gain, l))

    width, rows = carried.shape
    outs = [array((width, rows), F32), array((width + EXTRA, rows), BF16)]
    return local(kernel, outs, carried, *parts, gain)


def last_block(carried, parts, seqs, length):
    def kernel(carried, a, b, c, d, out):
        out[...] = added(carried, (a, b, c, d)).T.astype(BF16).reshape(out.shape)

    out = array((seqs, length, carried.shape[0]), BF16)
    return local(kernel, out, carried, *parts)


def joined(mine, other):
    seqs, length, width = mine.shape

    def kernel(mine, other, out):
        core, _, _ = position()
        out[pl.ds(core * seqs, seqs)] = mine[...]
        out[pl.ds((1 - core) * seqs, seqs)] = other[...]

    return local(kernel, array((2 * seqs, length, width), BF16), mine, other)


def products(unit, width, rows, operands, read, order):
    share = unit // SIDE
    stretches, count, step = rows

    def kernel(*refs):
        ins, outs, acc = refs[: len(operands)], refs[len(operands) : -1], refs[-1]
        _, _, second = position()
        for h in range(stretches):
            cut = slice(h * step, (h + 1) * step)
            total, squares = 0.0, 0.0
            for weights, acts, extra in read(ins, h):
                total = total + jnp.dot(weights, acts, preferred_element_type=F32)
                extra = extra.astype(F32)
                squares = squares + extra[0:1] + extra[1:2]
            acc[:, cut] = total
            squares = split_rows(squares)
            for out in outs:
                out[count // SIDE :, cut] = squares
        for d, out in zip(order, outs):
            start = pl.multiple_of((second ^ d) * share, 8)
            groups = [acc[pl.ds(start + g * unit, share)] for g in range(count // unit)]
            out[: count // SIDE] = jnp.concatenate(groups, axis=0).astype(BF16)

    tokens = stretches * step
    return local(
        kernel,
        [array((count // SIDE + EXTRA, tokens), BF16)] * len(order),
        *operands,
        flops=2 * count * SIDE * width * tokens,
        scratch=[pltpu.VMEM((count, tokens), F32)],
    )


def first_products(packs, unit, width, half, order):
    count = 2 * unit

    def read(refs, h):
        start = count + h * (width + EXTRA)
        for ref in refs:
            acts = ref[start : start + width]
            yield ref[:count], acts, ref[start + width : start + width + EXTRA]

    return products(unit, width, (2, count, half), packs, read, order)


def next_products(weights, acts, unit, width, half, order):
    n = len(weights)

    def read(refs, h):
        for w, a in zip(refs[:n], refs[n:]):
            yield w[...], a[:width], a[width:]

    return products(unit, width, (1, 4 * unit, half), [*weights, *acts], read, order)


def gated(parts, small, which, share, length):
    total, rows = parts[0].shape
    end = total - EXTRA

    def kernel(a, b, c, d, small, out):
        lane = lax.broadcasted_iota(jnp.int32, (share, length), 1)

        def conv(now, coef, k):
            one = jnp.where(lane >= 1, pltpu.roll(now, 1, 1), 0.0)
            two = jnp.where(lane >= 2, pltpu.roll(now, 2, 1), 0.0)
            early = coef[:, k + 3 : k + 4] + coef[:, k : k + 1] * two
            return early + coef[:, k + 1 : k + 2] * one + coef[:, k + 2 : k + 3] * now

        for s in range(rows // length):
            cut = slice(s * length, (s + 1) * length)
            a_, b_, c_, d_ = (p[:, cut].astype(F32) for p in (a, b, c, d))
            value = (a_ + b_) + (c_ + d_)
            row_squares = value[end : end + 1] + value[end + 1 : end + 2]
            inverse = lax.rsqrt(row_squares / D + eps)
            now = (value[:end] * inverse).astype(BF16).astype(F32)
            results = []
            for g, l in enumerate(which):
                coef = small[l, :share]
                gate = conv(now[2 * g * share : (2 * g + 1) * share], coef, 0)
                up = conv(now[(2 * g + 1) * share : (2 * g + 2) * share], coef, KERNEL + 1)
                results.append(gate / (1.0 + jnp.exp(-gate)) * up)
            out[:, cut] = jnp.concatenate(results, axis=0).astype(BF16)

    return local(kernel, array((end // 2, rows), BF16), *parts, small)


def collected(parts, share, ds):
    count, rows = parts[0].shape

    def kernel(*refs):
        out, buf = refs[SIDE], refs[SIDE + 1]
        _, _, second = position()
        for d, ref in zip(ds, refs):
            value = ref[...].astype(F32)
            for g in range(count // share):
                start = pl.multiple_of((g * SIDE + (second ^ d)) * share, 8)
                buf[pl.ds(start, share)] = value[g * share : (g + 1) * share]
        out[...] = buf[...].astype(BF16)

    out = array((SIDE * count, rows), BF16)
    scratch = [pltpu.VMEM((SIDE * count, rows), F32)]
    return local(kernel, out, *parts, scratch=scratch)


def mixed_down(sources, order):
    _, width, lanes = sources[0].shape
    m = len(sources)

    def kernel(*refs):
        _, first, _ = position()
        for d, out in zip(order, refs[m:]):
            for g in range(m):
                out[:, g * lanes : (g + 1) * lanes] = refs[g][first ^ d]

    outs = [array((width, m * lanes), BF16)] * len(order)
    return local(kernel, outs, *sources)


def spread(weights, groups, lanes, block):
    width = weights[0].shape[0]
    rows, tokens = block.shape
    n, unit = len(weights), rows // len(groups)

    def kernel(*refs):
        for w, out in zip(refs[:n], refs[n + 1 :]):
            total = 0.0
            for i, g in enumerate(groups):
                total = total + jnp.dot(
                    w[:, g * lanes : g * lanes + unit],
                    refs[n][i * unit : (i + 1) * unit],
                    preferred_element_type=F32,
                )
            out[...] = total.astype(BF16)

    flops = 2 * n * width * rows * tokens
    outs = [array((width, tokens), BF16)] * n
    return local(kernel, outs, *weights, block, flops=flops)


def summed(parts, dtypes):
    width, tokens = parts[0].shape
    step = tokens // len(dtypes)

    def kernel(a, b, c, d, *outs):
        for h, out in enumerate(outs):
            a_, b_, c_, d_ = (p[:, h * step : (h + 1) * step].astype(F32) for p in (a, b, c, d))
            out[...] = ((a_ + b_) + (c_ + d_)).astype(out.dtype)

    return local(kernel, [array((width, step), t) for t in dtypes], *parts)


def paired(mine, other):
    def kernel(mine, other, out):
        out[...] = (mine[...] + other[...].astype(F32)).astype(BF16)

    return local(kernel, array(mine.shape, BF16), mine, other)


def after(values, *earlier):
    return lax.optimization_barrier((values, *earlier))[0]


def per_device(
    tokens, norm_gain, gate_weight, up_weight, gate_taps, up_taps, gate_bias, up_bias, down_weight
):
    seqs, length, width = tokens.shape
    half = seqs // 2 * length
    unit = gate_weight.shape[2] // SIDE
    share = unit // SIDE
    every = tuple(range(SIDE))

    *packs, carried = first_pack(tokens, norm_gain, gate_weight, up_weight, every)
    mine = turn_in(gate_weight, up_weight, 1)
    turned = mixed(mine, to_twin(mine), every)
    downs = []
    for l in range(LAYERS):
        downs.append(turn_down(down_weight, l))
    lanes = downs[0].shape[2]
    downs = [mixed_down(downs[:1], every), mixed_down([downs[1], to_twin(downs[1])], every)]
    small = pack_small(gate_taps, up_taps, gate_bias, up_bias)
    small = turn_small(small, to_twin(small))
    got = moved(first_move, packs)
    got = after(got, downs, turned, small)
    got = [packs[0], *(got[d] for d in every[1:])]
    late = moved(first_move, downs[0])
    late = [downs[0][0], late[1], late[2], late[3]]
    parts = first_products(got, unit, width, half, every)
    for l in range(LAYERS):
        got = moved(second_move, parts)
        which = (0,) if l == 0 else (1, LAYERS + 1)
        hidden = gated([parts[0], got[1], got[2], got[3]], small, which, share, length)
        got = moved(second_move, [hidden] * SIDE)
        block = collected([hidden, got[1], got[2], got[3]], share, every)
        branch = spread(late, range(l + 1), lanes, block)
        got = moved(first_move, branch)
        got = [branch[0], got[1], got[2], got[3]]
        if l == 0:
            weights = moved(first_move, after(turned, block))
            weights = [turned[0], weights[1], weights[2], weights[3]]
            mine, twins = summed(got, [F32, BF16])
            branch = paired(mine, to_twin(twins))
        else:
            (branch,) = summed(got, [BF16])
        got = moved(x_move, [branch] * SIDE)
        got = [branch, got[1], got[2], got[3]]
        if l == 0:
            carried, acts = next_block(carried, got, norm_gain, l + 1)
            got = moved(first_move, [acts] * SIDE)
            got = [acts, got[1], got[2], got[3]]
            late = moved(first_move, after(downs[1], acts))
            late = [downs[1][0], late[1], late[2], late[3]]
            parts = next_products(weights, got, unit, width, half, every)
    mine = last_block(carried, got, seqs // 2, length)
    return joined(mine, to_twin(mine))


def solution(mesh):
    in_specs = (
        P(None, None, "ra"),
        P(None, "ra"),
        P(None, "ra", "cb"),
        P(None, "ra", "cb"),
        P(None, None, "cb"),
        P(None, None, "cb"),
        P(None, "cb"),
        P(None, "cb"),
        P(None, "cb", "ra"),
    )
    out_specs = P(None, None, "ra")

    return jax.shard_map(
        per_device, mesh=mesh, in_specs=in_specs, out_specs=out_specs, check_vma=False
    )
```

```python
import jax
import jax.numpy as jnp
from jax import lax
from jax.experimental import pallas as pl
from jax.experimental.pallas import tpu as pltpu
from jax.sharding import PartitionSpec as P


D = 4096
KERNEL = 3
LAYERS = 2
SIDE = 4
EXTRA = 8
AXES = ("ra", "cb")
BF16 = jnp.bfloat16
F32 = jnp.float32

eps = 1e-06
resid_scale = 0.5


def pairs(move):
    out = []
    for z in range(SIDE):
        for y in range(SIDE):
            for x in range(SIDE):
                for core in range(2):
                    to_z, to_y, to_x, to_core = move(z, y, x, core)
                    here = ((z * SIDE + y) * SIDE + x) * 2 + core
                    there = ((to_z * SIDE + to_y) * SIDE + to_x) * 2 + to_core
                    out.append((here, there))
    return out


def to_twin(value):
    return lax.ppermute(value, AXES, pairs(lambda z, y, x, c: (z, y, x, 1 - c)))


def first_move(d):
    return lambda z, y, x, c: (z, y ^ d, x, c) if c == 1 else (z ^ d, y, x, c)


def second_move(d):
    return lambda z, y, x, c: (z ^ d, y, x, c) if c == 1 else (z, y ^ d, x, c)


def x_move(d):
    return lambda z, y, x, c: (z, y, x ^ d, c)


def moved(move, values):
    got = {}
    for d in (1, 2, 3):
        got[d] = lax.ppermute(values[d], AXES, pairs(move(d)))
    return got


VMEM = pl.BlockSpec(memory_space=pltpu.VMEM)
HBM = pl.BlockSpec(memory_space=pltpu.HBM)


def position():
    cb, ra = lax.axis_index("cb"), lax.axis_index("ra")
    core, row, col = cb & 1, ra >> 2, ra & 3
    return core, jnp.where(core == 1, col, row), jnp.where(core == 1, row, col)


def local(kernel, outs, *args, flops=10**9, specs=None, scratch=()):
    many = isinstance(outs, list)
    moved = sum(a.size * a.dtype.itemsize for a in args)
    return pl.pallas_call(
        kernel,
        in_specs=specs or [VMEM] * len(args),
        out_specs=[VMEM] * len(outs) if many else VMEM,
        out_shape=outs,
        scratch_shapes=scratch,
        compiler_params=pltpu.CompilerParams(vmem_limit_bytes=16 * 2**20),
        cost_estimate=pl.CostEstimate(flops=flops, bytes_accessed=moved, transcendentals=0),
    )(*args)


def in_hbm(value):
    return pltpu.with_memory_space_constraint(value, pltpu.HBM)


def array(shape, dtype):
    return jax.ShapeDtypeStruct(shape, dtype)


def split_rows(row_sum):
    high = row_sum.astype(BF16).astype(F32)
    low = row_sum - high
    shape = (EXTRA, row_sum.shape[1])
    row = lax.broadcasted_iota(jnp.int32, shape, 0)
    high = jnp.broadcast_to(high, shape)
    low = jnp.broadcast_to(low, shape)
    return jnp.where(row == 0, high, jnp.where(row == 1, low, 0.0)).astype(BF16)


def column(gain, l):
    return jnp.broadcast_to(gain[l : l + 1], (8, gain.shape[1])).T[:, :1]


def store_acts(out, at_row, value, gain_column):
    width = value.shape[0]
    out[at_row : at_row + width] = (value * gain_column).astype(BF16)
    squares = split_rows(jnp.sum(value * value, axis=0, keepdims=True))
    out[at_row + width : at_row + width + EXTRA] = squares


def fetched(refs, bufs, sems):
    copies = [pltpu.make_async_copy(r, b, sems.at[i]) for i, (r, b) in enumerate(zip(refs, bufs))]
    for c in copies:
        c.start()
    return copies


def store_quarter(turns, q, out):
    quarter = turns[0].shape[0] // SIDE
    start = pl.multiple_of(q * quarter, 16)
    for i, turn in enumerate(turns):
        out[i * quarter : (i + 1) * quarter] = turn[pl.ds(start, quarter)]


def turn_scratch(width, cols):
    return [
        pltpu.VMEM((width, cols), BF16),
        pltpu.VMEM((width, cols), BF16),
        pltpu.VMEM((cols, width), BF16),
        pltpu.VMEM((cols, width), BF16),
    ]


def first_pack(tokens, gain, gate_weight, up_weight, order):
    seqs, length, width = tokens.shape
    cols = gate_weight.shape[2]
    half = seqs // 2 * length
    quarter = cols // 2
    n = len(order)

    def kernel(tokens, gain, gate, up, *refs):
        outs, carried = refs[:n], refs[n]
        gate_buf, up_buf, *turns, token_buf, gain_buf, sems = refs[n + 1 :]
        core, first, _ = position()
        copies = fetched(
            (tokens, gain, gate.at[0], up.at[0]), (token_buf, gain_buf, gate_buf, up_buf), sems
        )
        copies[0].wait()
        copies[1].wait()
        gain_column = column(gain_buf, 0)
        for h in range(2):
            place = core ^ h
            mine = token_buf[pl.ds(place * (seqs // 2), seqs // 2)].reshape(half, width)
            value = mine.astype(F32).T
            if h == 0:
                carried[...] = value
            for out in outs:
                store_acts(out, quarter + h * (width + EXTRA), value, gain_column)
        for c, buf, turn in zip(copies[2:], (gate_buf, up_buf), turns):
            c.wait()
            turn[...] = buf[...].T
        for d, out in zip(order, outs):
            store_quarter(turns, first ^ d, out)

    outs = [array((quarter + 2 * (width + EXTRA), width), BF16)] * n
    outs.append(array((width, half), F32))
    return local(
        kernel,
        outs,
        *map(in_hbm, (tokens, gain, gate_weight, up_weight)),
        specs=[HBM] * 4,
        scratch=[
            *turn_scratch(width, cols),
            pltpu.VMEM(tokens.shape, BF16),
            pltpu.VMEM(gain.shape, F32),
            pltpu.SemaphoreType.DMA((4,)),
        ],
    )


def turn_in(gate_weight, up_weight, l):
    _, width, cols = gate_weight.shape
    quarter = cols // 2

    def kernel(gate, up, out, gate_buf, up_buf, *rest):
        *turns, sems = rest
        copies = fetched((gate.at[l], up.at[l]), (gate_buf, up_buf), sems)
        for c, buf, turn in zip(copies, (gate_buf, up_buf), turns):
            c.wait()
            turn[...] = buf[...].T
        for q in range(SIDE):
            store_quarter(turns, q, out.at[q * quarter : (q + 1) * quarter])

    return local(
        kernel,
        array((SIDE * quarter, width), BF16),
        *map(in_hbm, (gate_weight, up_weight)),
        specs=[HBM, HBM],
        scratch=[*turn_scratch(width, cols), pltpu.SemaphoreType.DMA((2,))],
    )


def mixed(mine, twins, order):
    rows, width = mine.shape
    quarter = rows // SIDE

    def kernel(mine, twins, *outs):
        _, first, _ = position()
        for d, out in zip(order, outs):
            start = pl.multiple_of((first ^ d) * quarter, 16)
            out[:quarter] = mine[pl.ds(start, quarter)]
            out[quarter:] = twins[pl.ds(start, quarter)]

    return local(kernel, [array((2 * quarter, width), BF16)] * len(order), mine, twins)


def turn_down(down_weight, l):
    _, cols, width = down_weight.shape
    quarter = cols // SIDE

    def kernel(weights, out, buf, sems):
        for c in fetched((weights.at[l],), (buf,), sems):
            c.wait()
        for q in range(SIDE):
            out[q, :, :quarter] = buf[q * quarter : (q + 1) * quarter].T

    return local(
        kernel,
        array((SIDE, width, pl.cdiv(quarter, 128) * 128), BF16),
        in_hbm(down_weight),
        specs=[HBM],
        scratch=[pltpu.VMEM((cols, width), BF16), pltpu.SemaphoreType.DMA((1,))],
    )


def pack_small(gate_taps, up_taps, gate_bias, up_bias):
    layers, cols = gate_bias.shape

    def kernel(gate_taps, up_taps, gate_bias, up_bias, out):
        for l in range(layers):
            rows = []
            for taps, bias in ((gate_taps, gate_bias), (up_taps, up_bias)):
                rows += [taps[t, l : l + 1] for t in range(KERNEL)] + [bias[l : l + 1]]
            out[l] = jnp.concatenate(rows, axis=0)

    turn = lambda taps: jnp.transpose(taps, (1, 0, 2))
    out = array((layers, 2 * (KERNEL + 1), cols), F32)
    return local(kernel, out, turn(gate_taps), turn(up_taps), gate_bias, up_bias)


def turn_small(mine, twins):
    layers, count, cols = mine.shape
    share = cols // (SIDE * SIDE)
    lanes = 128

    def kernel(mine, twins, out):
        _, first, second = position()
        shift = lax.rem(cols - (first * SIDE + second) * share, cols)
        for i, ref in enumerate((mine, twins)):
            for l in range(layers):
                out[i * layers + l] = pltpu.roll(ref[l], shift, 1)[:, :lanes].T

    return local(kernel, array((2 * layers, lanes, count), F32), mine, twins)


def added(carried, parts):
    a, b, c, d = (p[...].astype(F32) for p in parts)
    return resid_scale * carried[...] + ((a + b) + (c + d))


def next_block(carried, parts, gain, l):
    def kernel(carried, a, b, c, d, gain, out, acts):
        value = added(carried, (a, b, c, d))
        out[...] = value
        store_acts(acts, 0, value, column(gain, l))

    width, rows = carried.shape
    outs = [array((width, rows), F32), array((width + EXTRA, rows), BF16)]
    return local(kernel, outs, carried, *parts, gain)


def last_block(carried, parts, seqs, length):
    def kernel(carried, a, b, c, d, out):
        out[...] = added(carried, (a, b, c, d)).T.astype(BF16).reshape(out.shape)

    out = array((seqs, length, carried.shape[0]), BF16)
    return local(kernel, out, carried, *parts)


def joined(mine, other):
    seqs, length, width = mine.shape

    def kernel(mine, other, out):
        core, _, _ = position()
        out[pl.ds(core * seqs, seqs)] = mine[...]
        out[pl.ds((1 - core) * seqs, seqs)] = other[...]

    return local(kernel, array((2 * seqs, length, width), BF16), mine, other)


def accumulated(ins, read, h, total, squares):
    for weights, acts, extra in read(ins, h):
        total = total + jnp.dot(weights, acts, preferred_element_type=F32)
        extra = extra.astype(F32)
        squares = squares + extra[0:1] + extra[1:2]
    return total, squares


def begun(rows, operands, read):
    stretches, count, step = rows
    tokens = stretches * step

    def kernel(*refs):
        ins, (total, squares) = refs[:-2], refs[-2:]
        for h in range(stretches):
            cut = slice(h * step, (h + 1) * step)
            total[:, cut], row = accumulated(ins, read, h, 0.0, 0.0)
            squares[:, cut] = jnp.broadcast_to(row, (8, step))

    outs = [array((count, tokens), F32), array((8, tokens), F32)]
    return local(kernel, outs, *operands)


def products(unit, width, rows, begin_with, operands, read, order):
    share = unit // SIDE
    stretches, count, step = rows
    n = len(operands)

    def kernel(*refs):
        ins, (start_total, start_squares), outs, acc = refs[:n], refs[n : n + 2], refs[n + 2 : -1], refs[-1]
        _, _, second = position()
        for h in range(stretches):
            cut = slice(h * step, (h + 1) * step)
            acc[:, cut], squares = accumulated(
                ins, read, h, start_total[:, cut], start_squares[0:1, cut]
            )
            squares = split_rows(squares)
            for out in outs:
                out[count // SIDE :, cut] = squares
        for d, out in zip(order, outs):
            start = pl.multiple_of((second ^ d) * share, 8)
            groups = [acc[pl.ds(start + g * unit, share)] for g in range(count // unit)]
            out[: count // SIDE] = jnp.concatenate(groups, axis=0).astype(BF16)

    tokens = stretches * step
    return local(
        kernel,
        [array((count // SIDE + EXTRA, tokens), BF16)] * len(order),
        *operands,
        *begin_with,
        flops=2 * count * SIDE * width * tokens,
        scratch=[pltpu.VMEM((count, tokens), F32)],
    )


def first_products(own, packs, unit, width, half, order):
    count = 2 * unit
    rows = (2, count, half)

    def read(refs, h):
        start = count + h * (width + EXTRA)
        for ref in refs:
            acts = ref[start : start + width]
            yield ref[:count], acts, ref[start + width : start + width + EXTRA]

    begin_with = begun(rows, [own], read)
    return products(unit, width, rows, begin_with, packs, read, order)


def next_products(own, weights, acts, unit, width, half, order):
    rows = (1, 4 * unit, half)

    def read(refs, h):
        n = len(refs) // 2
        for w, a in zip(refs[:n], refs[n:]):
            yield w[...], a[:width], a[width:]

    begin_with = begun(rows, own, read)
    return products(unit, width, rows, begin_with, [*weights, *acts], read, order)


def gated(parts, small, which, share, length):
    total, rows = parts[0].shape
    end = total - EXTRA

    def kernel(a, b, c, d, small, out):
        lane = lax.broadcasted_iota(jnp.int32, (share, length), 1)

        def conv(now, coef, k):
            one = jnp.where(lane >= 1, pltpu.roll(now, 1, 1), 0.0)
            two = jnp.where(lane >= 2, pltpu.roll(now, 2, 1), 0.0)
            early = coef[:, k + 3 : k + 4] + coef[:, k : k + 1] * two
            return early + coef[:, k + 1 : k + 2] * one + coef[:, k + 2 : k + 3] * now

        for s in range(rows // length):
            cut = slice(s * length, (s + 1) * length)
            a_, b_, c_, d_ = (p[:, cut].astype(F32) for p in (a, b, c, d))
            value = (a_ + b_) + (c_ + d_)
            row_squares = value[end : end + 1] + value[end + 1 : end + 2]
            inverse = lax.rsqrt(row_squares / D + eps)
            now = (value[:end] * inverse).astype(BF16).astype(F32)
            results = []
            for g, l in enumerate(which):
                coef = small[l, :share]
                gate = conv(now[2 * g * share : (2 * g + 1) * share], coef, 0)
                up = conv(now[(2 * g + 1) * share : (2 * g + 2) * share], coef, KERNEL + 1)
                results.append(gate / (1.0 + jnp.exp(-gate)) * up)
            out[:, cut] = jnp.concatenate(results, axis=0).astype(BF16)

    return local(kernel, array((end // 2, rows), BF16), *parts, small)


def collected(parts, share, ds):
    count, rows = parts[0].shape

    def kernel(*refs):
        out, buf = refs[SIDE], refs[SIDE + 1]
        _, _, second = position()
        for d, ref in zip(ds, refs):
            value = ref[...].astype(F32)
            for g in range(count // share):
                start = pl.multiple_of((g * SIDE + (second ^ d)) * share, 8)
                buf[pl.ds(start, share)] = value[g * share : (g + 1) * share]
        out[...] = buf[...].astype(BF16)

    out = array((SIDE * count, rows), BF16)
    scratch = [pltpu.VMEM((SIDE * count, rows), F32)]
    return local(kernel, out, *parts, scratch=scratch)


def mixed_down(sources, order):
    _, width, lanes = sources[0].shape
    m = len(sources)

    def kernel(*refs):
        _, first, _ = position()
        for d, out in zip(order, refs[m:]):
            for g in range(m):
                out[:, g * lanes : (g + 1) * lanes] = refs[g][first ^ d]

    outs = [array((width, m * lanes), BF16)] * len(order)
    return local(kernel, outs, *sources)


def spread(weights, groups, lanes, block):
    width = weights[0].shape[0]
    rows, tokens = block.shape
    n, unit = len(weights), rows // len(groups)

    def kernel(*refs):
        for w, out in zip(refs[:n], refs[n + 1 :]):
            total = 0.0
            for i, g in enumerate(groups):
                total = total + jnp.dot(
                    w[:, g * lanes : g * lanes + unit],
                    refs[n][i * unit : (i + 1) * unit],
                    preferred_element_type=F32,
                )
            out[...] = total.astype(BF16)

    flops = 2 * n * width * rows * tokens
    outs = [array((width, tokens), BF16)] * n
    return local(kernel, outs, *weights, block, flops=flops)


def summed(parts, dtypes):
    width, tokens = parts[0].shape
    step = tokens // len(dtypes)

    def kernel(a, b, c, d, *outs):
        for h, out in enumerate(outs):
            a_, b_, c_, d_ = (p[:, h * step : (h + 1) * step].astype(F32) for p in (a, b, c, d))
            out[...] = ((a_ + b_) + (c_ + d_)).astype(out.dtype)

    return local(kernel, [array((width, step), t) for t in dtypes], *parts)


def paired(mine, other):
    def kernel(mine, other, out):
        out[...] = (mine[...] + other[...].astype(F32)).astype(BF16)

    return local(kernel, array(mine.shape, BF16), mine, other)


def after(values, *earlier):
    return lax.optimization_barrier((values, *earlier))[0]


def per_device(
    tokens, norm_gain, gate_weight, up_weight, gate_taps, up_taps, gate_bias, up_bias, down_weight
):
    seqs, length, width = tokens.shape
    half = seqs // 2 * length
    unit = gate_weight.shape[2] // SIDE
    share = unit // SIDE
    every = tuple(range(SIDE))

    *packs, carried = first_pack(tokens, norm_gain, gate_weight, up_weight, every)
    mine = turn_in(gate_weight, up_weight, 1)
    turned = mixed(mine, to_twin(mine), every)
    downs = []
    for l in range(LAYERS):
        downs.append(turn_down(down_weight, l))
    lanes = downs[0].shape[2]
    downs = [mixed_down(downs[:1], every), mixed_down([downs[1], to_twin(downs[1])], every)]
    small = pack_small(gate_taps, up_taps, gate_bias, up_bias)
    small = turn_small(small, to_twin(small))
    got = moved(first_move, packs)
    got = after(got, downs, turned, small)
    got = [got[d] for d in every[1:]]
    late = moved(first_move, downs[0])
    late = [downs[0][0], late[1], late[2], late[3]]
    parts = first_products(packs[0], got, unit, width, half, every)
    for l in range(LAYERS):
        got = moved(second_move, parts)
        which = (0,) if l == 0 else (1, LAYERS + 1)
        hidden = gated([parts[0], got[1], got[2], got[3]], small, which, share, length)
        got = moved(second_move, [hidden] * SIDE)
        block = collected([hidden, got[1], got[2], got[3]], share, every)
        branch = [spread([w], range(l + 1), lanes, block)[0] for w in late[1:]]
        got = moved(first_move, [None, *branch])
        (mine,) = spread(late[:1], range(l + 1), lanes, block)
        got = [mine, got[1], got[2], got[3]]
        if l == 0:
            weights = moved(first_move, after(turned, block))
            weights = [turned[0], weights[1], weights[2], weights[3]]
            mine, twins = summed(got, [F32, BF16])
            branch = paired(mine, to_twin(twins))
        else:
            (branch,) = summed(got, [BF16])
        got = moved(x_move, [branch] * SIDE)
        got = [branch, got[1], got[2], got[3]]
        if l == 0:
            carried, acts = next_block(carried, got, norm_gain, l + 1)
            got = moved(first_move, [acts] * SIDE)
            got = [got[1], got[2], got[3]]
            late = moved(first_move, after(downs[1], acts))
            late = [downs[1][0], late[1], late[2], late[3]]
            own = [weights[0], acts]
            parts = next_products(own, weights[1:], got, unit, width, half, every)
    mine = last_block(carried, got, seqs // 2, length)
    return joined(mine, to_twin(mine))


def solution(mesh):
    in_specs = (
        P(None, None, "ra"),
        P(None, "ra"),
        P(None, "ra", "cb"),
        P(None, "ra", "cb"),
        P(None, None, "cb"),
        P(None, None, "cb"),
        P(None, "cb"),
        P(None, "cb"),
        P(None, "cb", "ra"),
    )
    out_specs = P(None, None, "ra")

    return jax.shard_map(
        per_device, mesh=mesh, in_specs=in_specs, out_specs=out_specs, check_vma=False
    )
```
